32 devices in a mesh: st: 16 (over z, y, x), tp: 2 (over core).
Axes of the slice: x: 2, y: 2, z: 4, core: 2. Of those that a mesh axis runs over, the one named last changes fastest.
Arguments:
- tokens: bfloat16 [4096, 2048], P('st'), may hold values from -6 to 6
- store: bfloat16 [64, 64, 2048], P('st'), may hold values from -6 to 6
- passage_ids: int32 [64, 4], P('st'), may hold values from 0 to 63, as said below
- w_query: bfloat16 [2048, 2048], P(None, 'tp'), may hold values from -0.125 to 0.125
- w_key: bfloat16 [2048, 512], P(None, 'tp'), may hold values from -0.125 to 0.125
- w_value: bfloat16 [2048, 512], P(None, 'tp'), may hold values from -0.125 to 0.125
- w_ret_query: bfloat16 [2048, 1024], P(None, 'tp'), may hold values from -0.125 to 0.125
- w_ret_key: bfloat16 [2048, 1024], P(None, 'tp'), may hold values from -0.125 to 0.125
- w_ret_value: bfloat16 [2048, 2048], P(None, 'tp'), may hold values from -0.125 to 0.125
- ret_rate: float32 [8], P('tp'), may hold values from 0.003 to 0.03
- ret_gain: float32 [2048], P('tp'), may hold values from 0.1 to 1.9
- gate_logit: float32 [2048], P('tp'), may hold values from -2 to 2
- out_grad: bfloat16 [4096, 2048], P('st', 'tp'), may hold values from -6 to 6
Outputs:
- grad_tokens: bfloat16 [4096, 2048], P(('st', 'tp'))
- grad_store: bfloat16 [64, 64, 2048], P(('st', 'tp'))
- grad_key_weight: float32 [2048, 512], P(None, 'tp')
The draws below stay inside these ranges and needn't reach their ends.
Inputs may be any that keep to these rules, and one draw needn't show every extreme that they name: `passage_ids`: passage p lies on index p // 4 of st. The rows of one device name exactly 1 passage of every owner, so the 4 passages of a block differ.
All inputs are finite; a program needn't handle non-finite values.
Results may differ from the reference program's by a relative error of at most 0.012.
Values may be sent and summed in bfloat16 or wider, within the bound.
A program may use at most 192 MiB of HBM per device.

```python
import math
import jax
import jax.numpy as jnp
from jax import lax

D = 2048
HEADS = 8
HEAD = 256
KV_HEADS = 2
RET_HEADS = 8
RET_KEY = 128
RET_VALUE = 256
BLK = 64
KP = 4
PLEN = 64
PASS_DEV = 4
TOK_DEV = 256
TOKENS = 4096
BLOCKS = 64
PASSAGES = 64
N_ST = 16


def draw_passage_ids(key, part):

    def for_reader(reader):
        stream = jax.random.fold_in(jax.random.fold_in(key, 7), reader)
        first, second, third = jax.random.split(stream, 3)
        owner = jax.random.permutation(first, N_ST).astype(jnp.int32)
        local = jnp.minimum(jax.random.randint(second, (N_ST,), 0, PASS_DEV), jax.random.randint(third, (N_ST,), 0, PASS_DEV))
        return (owner * PASS_DEV + local).astype(jnp.int32)
    every = jax.vmap(for_reader)(jnp.arange(N_ST, dtype=jnp.int32))
    return every.reshape(BLOCKS, KP)


def shard_levels(own_key, dims, pieces, least, top_value):
    gain = 1.0
    for axis_at, blocks in pieces:
        steps = jax.random.uniform(jax.random.fold_in(jax.random.fold_in(own_key, 6), axis_at), (blocks,), jnp.float32, least / len(pieces), top_value / len(pieces))
        gain = gain * jnp.repeat(jnp.exp(steps), dims[axis_at] // blocks).reshape((-1,) + (1,) * (len(dims) - 1 - axis_at))
    return gain


def scatter_about(rng, extent, spread, bound, pieces=(), kind=jnp.bfloat16):
    values = jax.random.normal(rng, extent, jnp.float32) * spread
    if len(pieces) > 0:
        values = shard_levels(rng, extent, pieces, -0.22, 0.18) * values
    return jnp.clip(values, min=-bound, max=bound).astype(kind)


def setup_inputs(seed: int = 0) -> dict:
    key_list = jax.random.split(jax.random.key(seed), 14)
    tokens = scatter_about(key_list[0], (TOKENS, D), 1.0, 6.0, ((0, 16),))
    store = scatter_about(key_list[1], (PASSAGES, PLEN, D), 1.0, 6.0, ((0, 16),))
    passage_ids = draw_passage_ids(jax.random.fold_in(key_list[13], 71), 0)
    w_query = scatter_about(key_list[3], (D, HEADS * HEAD), D ** -0.5, 0.125, ((1, 2),))
    w_key = scatter_about(key_list[4], (D, KV_HEADS * HEAD), D ** -0.5, 0.125, ((1, 2),))
    w_value = scatter_about(key_list[5], (D, KV_HEADS * HEAD), D ** -0.5, 0.125, ((1, 2),))
    w_ret_query = scatter_about(key_list[6], (D, RET_HEADS * RET_KEY), D ** -0.5, 0.125, ((1, 2),))
    w_ret_key = scatter_about(key_list[7], (D, RET_HEADS * RET_KEY), D ** -0.5, 0.125, ((1, 2),))
    w_ret_value = scatter_about(key_list[8], (D, RET_HEADS * RET_VALUE), D ** -0.5, 0.125, ((1, 2),))
    ret_rate = jnp.clip(jnp.exp(math.log(0.03) - 2.3025851 * jax.random.uniform(key_list[9], (RET_HEADS,), jnp.float32) ** shard_levels(key_list[9], (RET_HEADS,), ((0, 2),), -0.2, 0.2)), 0.003, 0.03)
    ret_gain = jnp.clip(1.0 + 0.18 * jax.random.normal(key_list[10], (D,), jnp.float32), 0.1, 1.9)
    gate_logit = jnp.clip(jax.random.uniform(key_list[11], (D,), jnp.float32, -2.0, 2.0) * shard_levels(key_list[11], (D,), ((0, 2),), -0.4, 0.0), -2.0, 2.0)
    out_grad = scatter_about(key_list[12], (TOKENS, D), 1.0, 6.0, ((0, 16), (1, 2)))
    return {"tokens": tokens, "store": store, "passage_ids": passage_ids, "w_query": w_query, "w_key": w_key, "w_value": w_value, "w_ret_query": w_ret_query, "w_ret_key": w_ret_key, "w_ret_value": w_ret_value, "ret_rate": ret_rate, "ret_gain": ret_gain, "gate_logit": gate_logit, "out_grad": out_grad}


EPSILON = 1.0
HIGH = lax.Precision.HIGHEST

def rounded(values):
    return lax.optimization_barrier(values.astype(jnp.bfloat16)).astype(jnp.float32)

def retention_grads(query_rows, key_rows, value_rows, rates, gains, cotangent):
    length = query_rows.shape[0]
    heads = rates.shape[0]
    queries = query_rows.astype(jnp.float32).reshape(length, heads, -1)
    keyset = key_rows.astype(jnp.float32).reshape(length, heads, -1)
    values = value_rows.astype(jnp.float32).reshape(length, heads, -1)
    positions = jnp.arange(length, dtype=jnp.float32)
    distance = positions[:, None] - positions[None, :]
    damping = jnp.where(distance >= 0.0, jnp.exp(-rates[:, None, None] * jnp.maximum(distance, 0.0)), 0.0) * queries.shape[-1] ** (-0.5)
    raw = jnp.einsum('thd,shd->hts', queries, keyset, precision=HIGH)
    weights = rounded(raw * damping)
    mixed = jnp.einsum('hts,she->the', weights, values, precision=HIGH)
    inverse = lax.rsqrt(lax.optimization_barrier(jnp.mean(mixed * mixed, axis=-1, keepdims=True)) + EPSILON)
    scaled = cotangent.astype(jnp.float32).reshape(length, heads, -1) * gains.reshape(heads, -1)
    inner = lax.optimization_barrier(jnp.mean(scaled * mixed, axis=-1, keepdims=True))
    grad_mixed = rounded(inverse * scaled - inverse * inverse * inverse * mixed * inner)
    grad_weights = rounded(jnp.einsum('the,she->hts', grad_mixed, values, precision=HIGH) * damping)
    grad_first = jnp.einsum('hts,shd->thd', grad_weights, keyset, precision=HIGH).astype(jnp.bfloat16).reshape(length, -1)
    grad_second = jnp.einsum('hts,thd->shd', grad_weights, queries, precision=HIGH).astype(jnp.bfloat16).reshape(length, -1)
    grad_third = jnp.einsum('hts,the->she', weights, grad_mixed, precision=HIGH).astype(jnp.bfloat16).reshape(length, -1)
    return (grad_first, grad_second, grad_third)

def reference(tokens, store, passage_ids, w_query, w_key, w_value, w_ret_query, w_ret_key, w_ret_value, ret_rate, ret_gain, gate_logit, out_grad):
    count, plen, width = store.shape
    kv_width = w_key.shape[1]
    kv_heads = kv_width // HEAD
    group = w_query.shape[1] // HEAD // kv_heads
    flat_store = store.reshape(count * plen, width)
    key_table = jnp.dot(flat_store, w_key, preferred_element_type=jnp.float32).astype(jnp.bfloat16).reshape(count, plen, kv_width)
    value_table = jnp.dot(flat_store, w_value, preferred_element_type=jnp.float32).astype(jnp.bfloat16).reshape(count, plen, kv_width)
    gate = jax.nn.sigmoid(gate_logit)
    blocks_dev = TOK_DEV // BLK
    seq_tokens = tokens.reshape(N_ST, TOK_DEV, width)
    seq_ids = passage_ids.reshape(N_ST, blocks_dev * KP)
    seq_grad = out_grad.reshape(N_ST, TOK_DEV, width)
    factor = HEAD ** (-0.5)

    def per_sequence(carry, inputs):
        rows, ids, grad_rows = inputs
        query_bf = jnp.dot(rows, w_query, preferred_element_type=jnp.float32).astype(jnp.bfloat16)
        keys = key_table[ids].reshape(blocks_dev, KP * plen, kv_heads, HEAD).astype(jnp.float32)
        values = value_table[ids].reshape(blocks_dev, KP * plen, kv_heads, HEAD).astype(jnp.float32)
        queries = query_bf.reshape(blocks_dev, BLK, kv_heads, group, HEAD).astype(jnp.float32)
        scores = jnp.einsum('btkgd,bskd->bkgts', queries, keys, precision=HIGH) * factor
        expo = jnp.exp(scores)
        probs = expo / lax.optimization_barrier(jnp.sum(expo, axis=-1, keepdims=True))
        probs_bf = rounded(probs)
        attn = jnp.einsum('bkgts,bskd->btkgd', probs_bf, values, precision=HIGH)
        grad_attn = grad_rows.astype(jnp.float32).reshape(blocks_dev, BLK, kv_heads, group, HEAD) * gate.reshape(kv_heads, group, HEAD)
        grad_attn_bf = rounded(grad_attn)
        grad_probs = jnp.einsum('btkgd,bskd->bkgts', grad_attn_bf, values, precision=HIGH)
        delta = jnp.einsum('btkgd,btkgd->bkgt', grad_attn, attn, precision=HIGH)
        grad_scores = rounded(probs * (grad_probs - delta[..., None]) * factor)
        grad_query = jnp.einsum('bkgts,bskd->btkgd', grad_scores, keys, precision=HIGH).astype(jnp.bfloat16).reshape(TOK_DEV, -1)
        grad_keys = jnp.einsum('bkgts,btkgd->bskd', grad_scores, queries, precision=HIGH).astype(jnp.bfloat16).reshape(blocks_dev * KP, plen, kv_width)
        grad_values = jnp.einsum('bkgts,btkgd->bskd', probs_bf, grad_attn_bf, precision=HIGH).astype(jnp.bfloat16).reshape(blocks_dev * KP, plen, kv_width)
        ret_query = jnp.dot(rows, w_ret_query, preferred_element_type=jnp.float32).astype(jnp.bfloat16)
        ret_key = jnp.dot(rows, w_ret_key, preferred_element_type=jnp.float32).astype(jnp.bfloat16)
        ret_value = jnp.dot(rows, w_ret_value, preferred_element_type=jnp.float32).astype(jnp.bfloat16)
        grad_rq, grad_rk, grad_rv = retention_grads(ret_query, ret_key, ret_value, ret_rate, ret_gain, grad_rows)
        grad_rows_out = (jnp.dot(grad_query, w_query.T, preferred_element_type=jnp.float32) + jnp.dot(grad_rq, w_ret_query.T, preferred_element_type=jnp.float32) + jnp.dot(grad_rk, w_ret_key.T, preferred_element_type=jnp.float32) + jnp.dot(grad_rv, w_ret_value.T, preferred_element_type=jnp.float32)).astype(jnp.bfloat16)
        slot_rows = store[ids].reshape(-1, width)
        carry = carry + jnp.dot(slot_rows.T, grad_keys.reshape(-1, kv_width), preferred_element_type=jnp.float32)
        return (carry, (grad_rows_out, grad_keys, grad_values))
    start = jnp.zeros((width, kv_width), jnp.float32)
    key_weight_grad, outputs = lax.scan(per_sequence, start, (seq_tokens, seq_ids, seq_grad))
    grad_rows_all, slot_keys, slot_values = outputs
    flat_ids = passage_ids.reshape(-1).astype(jnp.int32)
    passage_keys = jax.ops.segment_sum(slot_keys.reshape(-1, plen * kv_width).astype(jnp.float32), flat_ids, num_segments=count)
    passage_values = jax.ops.segment_sum(slot_values.reshape(-1, plen * kv_width).astype(jnp.float32), flat_ids, num_segments=count)
    keys_bf = passage_keys.astype(jnp.bfloat16).reshape(count * plen, kv_width)
    values_bf = passage_values.astype(jnp.bfloat16).reshape(count * plen, kv_width)
    grad_store = (jnp.dot(keys_bf, w_key.T, preferred_element_type=jnp.float32) + jnp.dot(values_bf, w_value.T, preferred_element_type=jnp.float32)).astype(jnp.bfloat16).reshape(count, plen, width)
    return (grad_rows_all.reshape(-1, width), grad_store, key_weight_grad)
```

```python
import functools

import jax
import jax.numpy as jnp
from jax import lax
from jax.experimental import pallas as pl
from jax.experimental.pallas import tpu as pltpu
from jax.sharding import PartitionSpec as P

HEAD = 256
BLK = 64
KP = 4
MOST = 1


EPSILON = 1.0


def retention_grads(query_rows, key_rows, value_rows, rates, gains, cotangent):
    length = query_rows.shape[0]
    heads = rates.shape[0]
    queries = query_rows.reshape(length, heads, -1)
    keyset = key_rows.reshape(length, heads, -1)
    values = value_rows.reshape(length, heads, -1)
    positions = jnp.arange(length, dtype=jnp.float32)
    distance = positions[:, None] - positions[None, :]
    damping = jnp.where(
        distance >= 0.0, jnp.exp(-rates[:, None, None] * jnp.maximum(distance, 0.0)), 0.0
    ) * queries.shape[-1] ** (-0.5)
    raw = jnp.einsum("thd,shd->hts", queries, keyset, preferred_element_type=jnp.float32)
    weights = (raw * damping).astype(jnp.bfloat16)
    mixed = jnp.einsum("hts,she->the", weights, values, preferred_element_type=jnp.float32)
    inverse = lax.rsqrt(jnp.mean(mixed * mixed, axis=-1, keepdims=True) + EPSILON)
    scaled = cotangent.astype(jnp.float32).reshape(length, heads, -1) * gains.reshape(heads, -1)
    inner = jnp.mean(scaled * mixed, axis=-1, keepdims=True)
    grad_mixed = (inverse * scaled - inverse * inverse * inverse * mixed * inner).astype(
        jnp.bfloat16
    )
    grad_weights = (
        jnp.einsum("the,she->hts", grad_mixed, values, preferred_element_type=jnp.float32) * damping
    ).astype(jnp.bfloat16)
    grad_first = (
        jnp.einsum("hts,shd->thd", grad_weights, keyset, preferred_element_type=jnp.float32)
        .astype(jnp.bfloat16)
        .reshape(length, -1)
    )
    grad_second = (
        jnp.einsum("hts,thd->shd", grad_weights, queries, preferred_element_type=jnp.float32)
        .astype(jnp.bfloat16)
        .reshape(length, -1)
    )
    grad_third = (
        jnp.einsum("hts,the->she", weights, grad_mixed, preferred_element_type=jnp.float32)
        .astype(jnp.bfloat16)
        .reshape(length, -1)
    )
    return (grad_first, grad_second, grad_third)


def against_rows(left, weight):
    return lax.dot_general(
        left, weight, (((1,), (1,)), ((), ())), preferred_element_type=jnp.float32
    )


def across_rows(left, right):
    return lax.dot_general(
        left, right, (((0,), (0,)), ((), ())), preferred_element_type=jnp.float32
    )


def per_device_plain(
    tokens,
    store,
    passage_ids,
    w_query,
    w_key,
    w_value,
    w_ret_query,
    w_ret_key,
    w_ret_value,
    ret_rate,
    ret_gain,
    gate_logit,
    out_grad,
):
    owners = lax.axis_size("st")
    pass_dev, plen, width = store.shape
    length = tokens.shape[0]
    kv_width = w_key.shape[1]
    kv_local = kv_width // HEAD
    group = w_query.shape[1] // HEAD // kv_local
    blocks = length // BLK
    slot_ids = passage_ids.reshape(-1)
    slot_count = slot_ids.shape[0]
    slot_owner = slot_ids // pass_dev
    slot_local = slot_ids % pass_dev
    order = jnp.arange(slot_count, dtype=jnp.int32)
    same_owner = slot_owner[:, None] == slot_owner[None, :]
    rank = jnp.sum(same_owner & (order[None, :] < order[:, None]), axis=1)
    position = slot_owner * MOST + rank
    cells = owners * MOST
    placed = jnp.arange(cells, dtype=jnp.int32)[:, None] == position[None, :]
    request = (jnp.sum(jnp.where(placed, slot_local[None, :] + 1, 0), axis=1) - 1).reshape(
        owners, MOST
    )
    incoming = lax.all_to_all(request, "st", split_axis=0, concat_axis=0, tiled=True)
    wanted = incoming.reshape(-1)
    valid = wanted >= 0
    safe = jnp.maximum(wanted, 0)
    placed_bf = placed.astype(jnp.bfloat16)
    store_rows = store.reshape(-1, width)
    nothing = jnp.zeros((), jnp.bfloat16)
    own_kv = jnp.concatenate(
        [
            jnp.dot(store_rows, w_key, preferred_element_type=jnp.float32).astype(jnp.bfloat16),
            jnp.dot(store_rows, w_value, preferred_element_type=jnp.float32).astype(jnp.bfloat16),
        ],
        axis=1,
    ).reshape(pass_dev, plen, 2 * kv_width)
    reply = jnp.where(valid[:, None, None], own_kv[safe], nothing).reshape(
        owners, MOST, plen, 2 * kv_width
    )
    arrived = lax.all_to_all(reply, "st", split_axis=0, concat_axis=0, tiled=True)
    slot_kv = (
        across_rows(placed_bf, arrived.reshape(cells, -1))
        .astype(jnp.bfloat16)
        .reshape(slot_count, plen, 2 * kv_width)
    )
    factor = HEAD ** (-0.5)
    gate = jax.nn.sigmoid(gate_logit)
    query_bf = jnp.dot(tokens, w_query, preferred_element_type=jnp.float32).astype(jnp.bfloat16)
    queries = query_bf.reshape(blocks, BLK, kv_local, group, HEAD)
    keys = slot_kv[:, :, :kv_width].reshape(blocks, KP * plen, kv_local, HEAD)
    values = slot_kv[:, :, kv_width:].reshape(blocks, KP * plen, kv_local, HEAD)
    scores = (
        jnp.einsum("btkgd,bskd->bkgts", queries, keys, preferred_element_type=jnp.float32) * factor
    )
    expo = jnp.exp(scores)
    probs = expo / jnp.sum(expo, axis=-1, keepdims=True)
    probs_bf = probs.astype(jnp.bfloat16)
    attn = jnp.einsum("bkgts,bskd->btkgd", probs_bf, values, preferred_element_type=jnp.float32)
    grad_attn = out_grad.astype(jnp.float32).reshape(
        blocks, BLK, kv_local, group, HEAD
    ) * gate.reshape(kv_local, group, HEAD)
    grad_attn_bf = grad_attn.astype(jnp.bfloat16)
    grad_probs = jnp.einsum(
        "btkgd,bskd->bkgts", grad_attn_bf, values, preferred_element_type=jnp.float32
    )
    delta = jnp.moveaxis(jnp.sum(grad_attn * attn, axis=-1), 1, 3)
    grad_scores = (probs * (grad_probs - delta[..., None]) * factor).astype(jnp.bfloat16)
    grad_query = (
        jnp.einsum("bkgts,bskd->btkgd", grad_scores, keys, preferred_element_type=jnp.float32)
        .astype(jnp.bfloat16)
        .reshape(length, -1)
    )
    grad_keys = (
        jnp.einsum("bkgts,btkgd->bskd", grad_scores, queries, preferred_element_type=jnp.float32)
        .astype(jnp.bfloat16)
        .reshape(slot_count, plen, kv_width)
    )
    grad_values = (
        jnp.einsum("bkgts,btkgd->bskd", probs_bf, grad_attn_bf, preferred_element_type=jnp.float32)
        .astype(jnp.bfloat16)
        .reshape(slot_count, plen, kv_width)
    )
    slot_grad = jnp.concatenate([grad_keys, grad_values], axis=2)
    outgoing = (
        jnp.dot(placed_bf, slot_grad.reshape(slot_count, -1), preferred_element_type=jnp.float32)
        .astype(jnp.bfloat16)
        .reshape(owners, MOST, plen, 2 * kv_width)
    )
    returned = lax.all_to_all(outgoing, "st", split_axis=0, concat_axis=0, tiled=True)
    matched = (jnp.arange(pass_dev, dtype=jnp.int32)[:, None] == wanted[None, :]).astype(
        jnp.bfloat16
    )
    passage_grad = jnp.dot(
        matched, returned.reshape(cells, -1), preferred_element_type=jnp.float32
    ).reshape(pass_dev * plen, 2 * kv_width)
    key_grad = passage_grad[:, :kv_width]
    upper = key_grad.astype(jnp.bfloat16)
    lower = (key_grad - upper.astype(jnp.float32)).astype(jnp.bfloat16)
    key_term = across_rows(store_rows, upper) + across_rows(store_rows, lower)
    grad_key_weight = lax.psum(key_term, "st")
    passage_bf = passage_grad.astype(jnp.bfloat16)
    grad_store = lax.psum_scatter(
        (
            against_rows(passage_bf[:, :kv_width], w_key)
            + against_rows(passage_bf[:, kv_width:], w_value)
        ).astype(jnp.bfloat16),
        "tp",
        scatter_dimension=0,
        tiled=True,
    ).astype(jnp.float32)
    grad_store = grad_store.astype(jnp.bfloat16).reshape(-1, plen, width)
    ret_query = jnp.dot(tokens, w_ret_query, preferred_element_type=jnp.float32).astype(
        jnp.bfloat16
    )
    ret_key = jnp.dot(tokens, w_ret_key, preferred_element_type=jnp.float32).astype(jnp.bfloat16)
    ret_value = jnp.dot(tokens, w_ret_value, preferred_element_type=jnp.float32).astype(
        jnp.bfloat16
    )
    grad_rq, grad_rk, grad_rv = retention_grads(
        ret_query, ret_key, ret_value, ret_rate, ret_gain, out_grad
    )
    total = against_rows(grad_query, w_query)
    total = total + against_rows(grad_rq, w_ret_query)
    total = total + against_rows(grad_rk, w_ret_key)
    grad_tokens = lax.psum_scatter(
        (total + against_rows(grad_rv, w_ret_value)).astype(jnp.bfloat16),
        "tp",
        scatter_dimension=0,
        tiled=True,
    )
    return (grad_tokens, grad_store, grad_key_weight)


PLANE = 4
HALVES = 2
TILE = 256
BF = jnp.bfloat16
F32 = jnp.float32
MESH = pl.DeviceIdType.MESH


def nn(a, b):
    return lax.dot_general(a, b, (((1,), (0,)), ((), ())), preferred_element_type=F32)


def nt(a, b):
    return lax.dot_general(a, b, (((1,), (1,)), ((), ())), preferred_element_type=F32)


def tn(a, b):
    return lax.dot_general(a, b, (((0,), (0,)), ((), ())), preferred_element_type=F32)


def fused_kernel(
    n,
    ids_ref,
    rate_ref,
    gain_ref,
    gate_ref,
    tokens_hbm,
    store_hbm,
    wq_hbm,
    wk_hbm,
    wv_hbm,
    wrq_hbm,
    wrk_hbm,
    wrv_hbm,
    og_hbm,
    gt_hbm,
    gs_hbm,
    gkw_hbm,
    tokens,
    store,
    wq,
    wk,
    wv,
    wrq,
    wrk,
    wrv,
    og,
    q,
    rq,
    rk,
    rv,
    gq,
    grq,
    grk,
    grv,
    total,
    gt,
    gt_in,
    gs,
    gs_in,
    own_kv,
    req_out,
    req_in,
    kv_out,
    kv_in,
    stage_k,
    stage_v,
    gk_out,
    gv_out,
    gk_in,
    gv_in,
    pk,
    pv,
    kt,
    p1_in,
    p1_sum,
    p2_in,
    kg,
    owner_of,
    slot_of,
    load_sem,
    out_sem,
    tp_send,
    tp_recv,
    req_send,
    req_recv,
    kv_send,
    kv_recv,
    gk_send,
    gk_recv,
    gv_send,
    gv_recv,
    p1_send,
    p1_recv,
    p2_send,
    p2_recv,
    p3_send,
    p3_recv,
    p4_send,
    p4_recv,
):
    me = lax.axis_index("st")
    tp = lax.axis_index("tp")
    length = tokens.shape[0]
    width = tokens.shape[1]
    plen = kv_in.shape[1]
    pass_dev = store.shape[0] // plen
    blocks = length // BLK
    slots = blocks * KP
    group = q.shape[1] // HEAD
    ret_heads = rate_ref.shape[0]
    depth = n // PLANE
    my_q = lax.rem(me, PLANE)
    my_z = lax.div(me, PLANE)
    half_tok = length // 2
    half_store = store.shape[0] // 2

    pairs = (
        (store_hbm, store),
        (wk_hbm, wk),
        (wv_hbm, wv),
        (tokens_hbm, tokens),
        (wrq_hbm, wrq),
        (wrk_hbm, wrk),
        (wrv_hbm, wrv),
        (og_hbm, og),
        (wq_hbm, wq),
    )
    loads = [pltpu.make_async_copy(a, b, load_sem.at[i]) for i, (a, b) in enumerate(pairs)]
    for load in loads:
        load.start()

    barrier = pltpu.get_barrier_semaphore()

    def greet(i, carry):
        pl.semaphore_signal(
            barrier, inc=1, device_id={"st": lax.rem(me + i, n)}, device_id_type=MESH
        )
        return carry

    lax.fori_loop(1, n, greet, 0)
    pl.semaphore_signal(barrier, inc=1, device_id={"tp": 1 - tp}, device_id_type=MESH)

    for s in range(slots):
        owner_of[s] = lax.div(ids_ref[s // KP, s % KP], pass_dev)

    def invert(o, carry):
        local = jnp.int32(0)
        where = jnp.int32(0)
        for s in range(slots):
            ident = ids_ref[s // KP, s % KP]
            hit = owner_of[s] == o
            local = jnp.where(hit, lax.rem(ident, pass_dev), local)
            where = jnp.where(hit, jnp.int32(s), where)
        slot_of[o] = where
        req_out[o] = jnp.full(req_out.shape[1:], local, jnp.int32)
        return carry

    lax.fori_loop(0, n, invert, 0)

    def exchange(out_ref, in_ref, send, recv, i):
        target = lax.rem(me + i, n)
        return pltpu.make_async_remote_copy(
            src_ref=out_ref.at[target],
            dst_ref=in_ref.at[me],
            send_sem=send.at[target],
            recv_sem=recv.at[me],
            device_id={"st": target},
            device_id_type=MESH,
        )

    def arrival(out_ref, in_ref, send, recv, i):
        source = lax.rem(me + i, n)
        return pltpu.make_async_remote_copy(
            src_ref=out_ref.at[source],
            dst_ref=in_ref.at[source],
            send_sem=send.at[source],
            recv_sem=recv.at[source],
            device_id={"st": source},
            device_id_type=MESH,
        )

    def start_all(*refs):
        def body(i, carry):
            exchange(*refs, i).start()
            return carry

        lax.fori_loop(1, n, body, 0)

    def wait_recv_all(*refs):
        def body(i, carry):
            arrival(*refs, i).wait_recv()
            return carry

        lax.fori_loop(1, n, body, 0)

    def wait_send_all(*refs):
        def body(i, carry):
            exchange(*refs, i).wait_send()
            return carry

        lax.fori_loop(1, n, body, 0)

    reqs = (req_out, req_in, req_send, req_recv)
    kvs = (kv_out, kv_in, kv_send, kv_recv)
    gks = (gk_out, gk_in, gk_send, gk_recv)
    gvs = (gv_out, gv_in, gv_send, gv_recv)

    pl.semaphore_wait(barrier, n)
    start_all(*reqs)
    req_in[me] = req_out[me]

    for load in loads[:3]:
        load.wait()
    own_kv[:, :HEAD] = nn(store[...], wk[...]).astype(BF)
    own_kv[:, HEAD:] = nn(store[...], wv[...]).astype(BF)
    wait_recv_all(*reqs)

    def names(r, p, lanes):
        row = jnp.where(req_in[r][0:1, :] == p, 1.0, 0.0).astype(F32)
        return jnp.concatenate([row] * (lanes // row.shape[1]), axis=1)

    def select(r, carry):
        chosen = jnp.zeros((plen, 2 * HEAD), F32)
        for p in range(pass_dev):
            chosen = chosen + names(r, p, 2 * HEAD) * own_kv[p * plen : (p + 1) * plen, :].astype(F32)
        kv_out[r] = chosen.astype(BF)
        return carry

    lax.fori_loop(0, n, select, 0)
    kv_in[me] = kv_out[me]
    start_all(*kvs)

    def project(w, out):
        def body(i, carry):
            cols = pl.ds(pl.multiple_of(i * TILE, TILE), TILE)
            out[:, cols] = nn(tokens[...], w[:, cols]).astype(BF)
            return carry

        lax.fori_loop(0, w.shape[1] // TILE, body, 0)

    loads[3].wait()
    for load, w, out in ((loads[4], wrq, rq), (loads[5], wrk, rk), (loads[6], wrv, rv)):
        load.wait()
        project(w, out)
    loads[7].wait()

    ret_key = rq.shape[1] // ret_heads
    ret_value = rv.shape[1] // ret_heads
    at_t = lax.broadcasted_iota(jnp.int32, (length, length), 0)
    at_s = lax.broadcasted_iota(jnp.int32, (length, length), 1)
    distance = (at_t - at_s).astype(F32)

    def retention(j, carry):
        kc = pl.ds(pl.multiple_of(j * ret_key, ret_key), ret_key)
        vc = pl.ds(pl.multiple_of(j * ret_value, ret_value), ret_value)
        damping = jnp.where(
            distance >= 0.0, jnp.exp(-rate_ref[j] * jnp.maximum(distance, 0.0)), 0.0
        ) * ret_key ** (-0.5)
        weights = (nt(rq[:, kc], rk[:, kc]) * damping).astype(BF)
        y = nn(weights, rv[:, vc])
        r = lax.rsqrt(jnp.mean(y * y, axis=1, keepdims=True) + EPSILON)
        c = og[:, vc].astype(F32) * gain_ref[:, vc]
        inner = jnp.mean(c * y, axis=1, keepdims=True)
        gy = (r * c - r * r * r * y * inner).astype(BF)
        gw = (nt(gy, rv[:, vc]) * damping).astype(BF)
        grq[:, kc] = nn(gw, rk[:, kc]).astype(BF)
        grk[:, kc] = tn(gw, rq[:, kc]).astype(BF)
        grv[:, vc] = tn(weights, gy).astype(BF)
        return carry

    lax.fori_loop(0, ret_heads, retention, 0)
    loads[8].wait()
    project(wq, q)

    def ret_total(i, carry):
        rows = pl.ds(pl.multiple_of(i * TILE, TILE), TILE)
        total[:, rows] = (
            nt(grq[...], wrq[rows, :]) + nt(grk[...], wrk[rows, :]) + nt(grv[...], wrv[rows, :])
        )
        return carry

    lax.fori_loop(0, width // TILE, ret_total, 0)

    wait_recv_all(*kvs)
    factor = HEAD ** (-0.5)

    def attend(b, carry):
        rows = pl.ds(pl.multiple_of(b * BLK, BLK), BLK)
        read = [kv_in[owner_of[b * KP + k]] for k in range(KP)]
        keys = jnp.concatenate([x[:, :HEAD] for x in read], axis=0)
        values = jnp.concatenate([x[:, HEAD:] for x in read], axis=0)
        cols = [slice(g * HEAD, (g + 1) * HEAD) for g in range(group)]
        queries = jnp.concatenate([q[rows, c] for c in cols], axis=0)
        expo = jnp.exp(nt(queries, keys) * factor)
        probs = expo / jnp.sum(expo, axis=1, keepdims=True)
        probs_bf = probs.astype(BF)
        attn = nn(probs_bf, values)
        grad_attn = jnp.concatenate(
            [
                og[rows, c].astype(F32) * (1.0 / (1.0 + jnp.exp(-gate_ref[:, c])))
                for c in cols
            ],
            axis=0,
        )
        grad_attn_bf = grad_attn.astype(BF)
        grad_probs = nt(grad_attn_bf, values)
        delta = jnp.sum(grad_attn * attn, axis=1, keepdims=True)
        scores = (probs * (grad_probs - delta) * factor).astype(BF)
        grad_query = nn(scores, keys).astype(BF)
        for g, c in enumerate(cols):
            gq[rows, c] = grad_query[g * BLK : (g + 1) * BLK, :]
        dk = tn(scores, queries).astype(BF)
        dv = tn(probs_bf, grad_attn_bf).astype(BF)
        for k in range(KP):
            stage_k[b * KP + k] = dk[k * plen : (k + 1) * plen, :]
            stage_v[b * KP + k] = dv[k * plen : (k + 1) * plen, :]
        return carry

    lax.fori_loop(0, blocks, attend, 0)

    def place(stage, out):
        def body(o, carry):
            out[o] = stage[slot_of[o]]
            return carry

        lax.fori_loop(0, n, body, 0)

    place(stage_k, gk_out)
    place(stage_v, gv_out)
    gk_in[me] = gk_out[me]
    gv_in[me] = gv_out[me]
    start_all(*gks)
    start_all(*gvs)

    def finish_total(i, carry):
        rows = pl.ds(pl.multiple_of(i * TILE, TILE), TILE)
        gt[:, rows] = (total[:, rows] + nt(gq[...], wq[rows, :])).astype(BF)
        return carry

    lax.fori_loop(0, width // TILE, finish_total, 0)

    def to_partner(out_ref, in_ref, half, at):
        return pltpu.make_async_remote_copy(
            src_ref=out_ref.at[pl.ds(pl.multiple_of((1 - tp) * half, half), half)],
            dst_ref=in_ref,
            send_sem=tp_send.at[at],
            recv_sem=tp_recv.at[at],
            device_id={"tp": 1 - tp},
            device_id_type=MESH,
        )

    def add_own(out_ref, in_ref, half):
        own = out_ref[pl.ds(pl.multiple_of(tp * half, half), half), :]
        in_ref[...] = (own.astype(F32) + in_ref[...].astype(F32)).astype(BF)

    token_swap = to_partner(gt, gt_in, half_tok, 0)
    token_swap.start()

    def gather_sum(in_ref, out_ref):
        for p in range(pass_dev):

            def body(r, acc):
                return acc + names(r, p, HEAD) * in_ref[r].astype(F32)

            acc = lax.fori_loop(0, n, body, jnp.zeros((plen, HEAD), F32))
            out_ref[p * plen : (p + 1) * plen, :] = acc.astype(BF)

    wait_recv_all(*gks)
    gather_sum(gk_in, pk)
    piece = kt.shape[1]
    per_tile = TILE // piece

    def key_term(i, carry):
        cols = pl.ds(pl.multiple_of(i * TILE, TILE), TILE)
        term = tn(store[:, cols], pk[...]).astype(BF)
        kt[pl.ds(i * per_tile, per_tile)] = term.reshape(per_tile, piece, HEAD)
        return carry

    lax.fori_loop(0, width // TILE, key_term, 0)

    def chunk(h, quarter):
        return pl.ds((h * PLANE + quarter) * depth, depth)

    def plane_reduce(h, i):
        other = lax.rem(my_q + i, PLANE)
        return pltpu.make_async_remote_copy(
            src_ref=kt.at[chunk(h, other)],
            dst_ref=p1_in.at[h, i - 1],
            send_sem=p1_send.at[h, i - 1],
            recv_sem=p1_recv.at[h, i - 1],
            device_id={"st": my_z * PLANE + other},
            device_id_type=MESH,
        )

    def column_reduce(h, i):
        other = lax.rem(my_z + i, depth)
        return pltpu.make_async_remote_copy(
            src_ref=p1_sum.at[h, other],
            dst_ref=p2_in.at[h, i - 1],
            send_sem=p2_send.at[h, i - 1],
            recv_sem=p2_recv.at[h, i - 1],
            device_id={"st": other * PLANE + my_q},
            device_id_type=MESH,
        )

    def column_gather(h, i, source):
        at = kg.at[(h * PLANE + my_q) * depth + source]
        return pltpu.make_async_remote_copy(
            src_ref=at,
            dst_ref=at,
            send_sem=p3_send.at[h, i - 1],
            recv_sem=p3_recv.at[h, i - 1],
            device_id={"st": lax.rem(my_z + i, depth) * PLANE + my_q},
            device_id_type=MESH,
        )

    def plane_gather(h, i, source):
        at = kg.at[chunk(h, source)]
        return pltpu.make_async_remote_copy(
            src_ref=at,
            dst_ref=at,
            send_sem=p4_send.at[h, i - 1],
            recv_sem=p4_recv.at[h, i - 1],
            device_id={"st": my_z * PLANE + lax.rem(my_q + i, PLANE)},
            device_id_type=MESH,
        )

    for h in range(HALVES):
        for i in range(1, PLANE):
            plane_reduce(h, i).start()

    token_swap.wait_recv()
    add_own(gt, gt_in, half_tok)
    token_out = pltpu.make_async_copy(gt_in, gt_hbm, out_sem.at[0])
    token_out.start()

    for h in range(HALVES):
        for i in range(1, PLANE):
            plane_reduce(h, i).wait_recv()
        acc = kt[chunk(h, my_q)].astype(F32)
        for i in range(1, PLANE):
            acc = acc + p1_in[h, i - 1].astype(F32)
        p1_sum[h] = acc.astype(BF)
        for i in range(1, depth):
            column_reduce(h, i).start()

    wait_recv_all(*gvs)
    gather_sum(gv_in, pv)

    def store_grad(i, carry):
        rows = pl.ds(pl.multiple_of(i * TILE, TILE), TILE)
        gs[:, rows] = (nt(pk[...], wk[rows, :]) + nt(pv[...], wv[rows, :])).astype(BF)
        return carry

    lax.fori_loop(0, width // TILE, store_grad, 0)
    store_swap = to_partner(gs, gs_in, half_store, 1)
    store_swap.start()

    for h in range(HALVES):
        for i in range(1, depth):
            column_reduce(h, i).wait_recv()
        acc = p1_sum[h, my_z].astype(F32)
        for i in range(1, depth):
            acc = acc + p2_in[h, i - 1].astype(F32)
        kg[(h * PLANE + my_q) * depth + my_z] = acc.astype(BF)
        for i in range(1, depth):
            column_gather(h, i, my_z).start()

    store_swap.wait_recv()
    add_own(gs, gs_in, half_store)
    store_out = pltpu.make_async_copy(gs_in, gs_hbm, out_sem.at[1])
    store_out.start()

    for h in range(HALVES):
        for i in range(1, depth):
            column_gather(h, i, lax.rem(my_z + depth - i, depth)).wait_recv()
        for i in range(1, PLANE):
            plane_gather(h, i, my_q).start()
    for h in range(HALVES):
        for i in range(1, PLANE):
            plane_gather(h, i, lax.rem(my_q + PLANE - i, PLANE)).wait_recv()
    weight_out = pltpu.make_async_copy(kg, gkw_hbm, out_sem.at[2])
    weight_out.start()

    wait_send_all(*reqs)
    wait_send_all(*kvs)
    wait_send_all(*gks)
    wait_send_all(*gvs)
    token_swap.wait_send()
    store_swap.wait_send()
    for h in range(HALVES):
        for i in range(1, PLANE):
            plane_reduce(h, i).wait_send()
            plane_gather(h, i, my_q).wait_send()
        for i in range(1, depth):
            column_reduce(h, i).wait_send()
            column_gather(h, i, my_z).wait_send()
    token_out.wait()
    store_out.wait()
    weight_out.wait()


def per_device(sizes, *args):
    (tokens, store, ids, wq, wk, wv, wrq, wrk, wrv, rate, gain, gate, og) = args
    n = sizes["st"]
    pass_dev, plen, width = store.shape
    length = tokens.shape[0]
    rows = pass_dev * plen
    weight_cols = sum(w.shape[1] for w in (wq, wk, wv, wrq, wrk, wrv))
    fits = (
        sizes["tp"] == 2
        and wk.shape[1] == HEAD
        and ids.size == n
        and n % PLANE == 0
        and width % (HALVES * n) == 0
        and TILE % (width // (HALVES * n)) == 0
        and width * weight_cols + n * plen * HEAD * 12 + length * width * 12 < 24 * 2**20
    )
    if not fits:
        return per_device_plain(*args)
    depth = n // PLANE
    piece = width // (HALVES * n)

    def vm(*shape, dtype=BF):
        return pltpu.VMEM(shape, dtype)

    any_spec = pl.BlockSpec(memory_space=pl.ANY)
    smem = pl.BlockSpec(memory_space=pltpu.SMEM)
    vmem = pl.BlockSpec(memory_space=pltpu.VMEM)
    dma = pltpu.SemaphoreType.DMA
    like = [vm(*x.shape) for x in (tokens,)] + [vm(rows, width)]
    like += [vm(*x.shape) for x in (wq, wk, wv, wrq, wrk, wrv, og)]
    qs = [vm(length, w.shape[1]) for w in (wq, wrq, wrk, wrv)]
    scratch = (
        like
        + qs
        + qs
        + [
            vm(length, width, dtype=F32),
            vm(length, width),
            vm(length // 2, width),
            vm(rows, width),
            vm(rows // 2, width),
            vm(rows, 2 * HEAD),
            vm(n, 8, 128, dtype=jnp.int32),
            vm(n, 8, 128, dtype=jnp.int32),
            vm(n, plen, 2 * HEAD),
            vm(n, plen, 2 * HEAD),
        ]
        + [vm(n, plen, HEAD)] * 6
        + [
            vm(rows, HEAD),
            vm(rows, HEAD),
            vm(HALVES * n, piece, HEAD),
            vm(HALVES, PLANE - 1, depth, piece, HEAD),
            vm(HALVES, depth, piece, HEAD),
            vm(HALVES, depth - 1, piece, HEAD),
            vm(HALVES * n, piece, HEAD),
            pltpu.SMEM((n,), jnp.int32),
            pltpu.SMEM((n,), jnp.int32),
            dma((9,)),
            dma((3,)),
            dma((2,)),
            dma((2,)),
        ]
        + [dma((n,))] * 8
        + [dma((HALVES, PLANE - 1))] * 2
        + [dma((HALVES, depth - 1))] * 4
        + [dma((HALVES, PLANE - 1))] * 2
    )
    grad_tokens, grad_store, grad_key = pl.pallas_call(
        functools.partial(fused_kernel, n),
        out_shape=(
            jax.ShapeDtypeStruct((length // 2, width), BF),
            jax.ShapeDtypeStruct((rows // 2, width), BF),
            jax.ShapeDtypeStruct((HALVES * n, piece, HEAD), BF),
        ),
        in_specs=[smem, smem, vmem, vmem] + [any_spec] * 9,
        out_specs=(any_spec, any_spec, any_spec),
        scratch_shapes=scratch,
        compiler_params=pltpu.CompilerParams(
            collective_id=0, has_side_effects=True, vmem_limit_bytes=60 * 2**20
        ),
    )(
        ids,
        rate,
        gain.reshape(1, -1),
        gate.reshape(1, -1),
        tokens,
        store.reshape(rows, width),
        wq,
        wk,
        wv,
        wrq,
        wrk,
        wrv,
        og,
    )
    return (
        grad_tokens,
        grad_store.reshape(pass_dev // 2, plen, width),
        grad_key.reshape(width, HEAD).astype(F32),
    )


def solution(mesh):
    return jax.shard_map(
        functools.partial(per_device, dict(mesh.shape)),
        mesh=mesh,
        in_specs=(
            P("st", None),
            P("st", None, None),
            P("st", None),
            P(None, "tp"),
            P(None, "tp"),
            P(None, "tp"),
            P(None, "tp"),
            P(None, "tp"),
            P(None, "tp"),
            P("tp"),
            P("tp"),
            P("tp"),
            P("st", "tp"),
        ),
        out_specs=(P(("st", "tp"), None), P(("st", "tp"), None, None), P(None, "tp")),
        check_vma=False,
    )
```

```python
import functools

import jax
import jax.numpy as jnp
from jax import lax
from jax.experimental import pallas as pl
from jax.experimental.pallas import tpu as pltpu
from jax.sharding import PartitionSpec as P

HEAD = 256
BLK = 64
KP = 4
MOST = 1


EPSILON = 1.0


def retention_grads(query_rows, key_rows, value_rows, rates, gains, cotangent):
    length = query_rows.shape[0]
    heads = rates.shape[0]
    queries = query_rows.reshape(length, heads, -1)
    keyset = key_rows.reshape(length, heads, -1)
    values = value_rows.reshape(length, heads, -1)
    positions = jnp.arange(length, dtype=jnp.float32)
    distance = positions[:, None] - positions[None, :]
    damping = jnp.where(
        distance >= 0.0, jnp.exp(-rates[:, None, None] * jnp.maximum(distance, 0.0)), 0.0
    ) * queries.shape[-1] ** (-0.5)
    raw = jnp.einsum("thd,shd->hts", queries, keyset, preferred_element_type=jnp.float32)
    weights = (raw * damping).astype(jnp.bfloat16)
    mixed = jnp.einsum("hts,she->the", weights, values, preferred_element_type=jnp.float32)
    inverse = lax.rsqrt(jnp.mean(mixed * mixed, axis=-1, keepdims=True) + EPSILON)
    scaled = cotangent.astype(jnp.float32).reshape(length, heads, -1) * gains.reshape(heads, -1)
    inner = jnp.mean(scaled * mixed, axis=-1, keepdims=True)
    grad_mixed = (inverse * scaled - inverse * inverse * inverse * mixed * inner).astype(
        jnp.bfloat16
    )
    grad_weights = (
        jnp.einsum("the,she->hts", grad_mixed, values, preferred_element_type=jnp.float32) * damping
    ).astype(jnp.bfloat16)
    grad_first = (
        jnp.einsum("hts,shd->thd", grad_weights, keyset, preferred_element_type=jnp.float32)
        .astype(jnp.bfloat16)
        .reshape(length, -1)
    )
    grad_second = (
        jnp.einsum("hts,thd->shd", grad_weights, queries, preferred_element_type=jnp.float32)
        .astype(jnp.bfloat16)
        .reshape(length, -1)
    )
    grad_third = (
        jnp.einsum("hts,the->she", weights, grad_mixed, preferred_element_type=jnp.float32)
        .astype(jnp.bfloat16)
        .reshape(length, -1)
    )
    return (grad_first, grad_second, grad_third)


def against_rows(left, weight):
    return lax.dot_general(
        left, weight, (((1,), (1,)), ((), ())), preferred_element_type=jnp.float32
    )


def across_rows(left, right):
    return lax.dot_general(
        left, right, (((0,), (0,)), ((), ())), preferred_element_type=jnp.float32
    )


def per_device_plain(
    tokens,
    store,
    passage_ids,
    w_query,
    w_key,
    w_value,
    w_ret_query,
    w_ret_key,
    w_ret_value,
    ret_rate,
    ret_gain,
    gate_logit,
    out_grad,
):
    owners = lax.axis_size("st")
    pass_dev, plen, width = store.shape
    length = tokens.shape[0]
    kv_width = w_key.shape[1]
    kv_local = kv_width // HEAD
    group = w_query.shape[1] // HEAD // kv_local
    blocks = length // BLK
    slot_ids = passage_ids.reshape(-1)
    slot_count = slot_ids.shape[0]
    slot_owner = slot_ids // pass_dev
    slot_local = slot_ids % pass_dev
    order = jnp.arange(slot_count, dtype=jnp.int32)
    same_owner = slot_owner[:, None] == slot_owner[None, :]
    rank = jnp.sum(same_owner & (order[None, :] < order[:, None]), axis=1)
    position = slot_owner * MOST + rank
    cells = owners * MOST
    placed = jnp.arange(cells, dtype=jnp.int32)[:, None] == position[None, :]
    request = (jnp.sum(jnp.where(placed, slot_local[None, :] + 1, 0), axis=1) - 1).reshape(
        owners, MOST
    )
    incoming = lax.all_to_all(request, "st", split_axis=0, concat_axis=0, tiled=True)
    wanted = incoming.reshape(-1)
    valid = wanted >= 0
    safe = jnp.maximum(wanted, 0)
    placed_bf = placed.astype(jnp.bfloat16)
    store_rows = store.reshape(-1, width)
    nothing = jnp.zeros((), jnp.bfloat16)
    own_kv = jnp.concatenate(
        [
            jnp.dot(store_rows, w_key, preferred_element_type=jnp.float32).astype(jnp.bfloat16),
            jnp.dot(store_rows, w_value, preferred_element_type=jnp.float32).astype(jnp.bfloat16),
        ],
        axis=1,
    ).reshape(pass_dev, plen, 2 * kv_width)
    reply = jnp.where(valid[:, None, None], own_kv[safe], nothing).reshape(
        owners, MOST, plen, 2 * kv_width
    )
    arrived = lax.all_to_all(reply, "st", split_axis=0, concat_axis=0, tiled=True)
    slot_kv = (
        across_rows(placed_bf, arrived.reshape(cells, -1))
        .astype(jnp.bfloat16)
        .reshape(slot_count, plen, 2 * kv_width)
    )
    factor = HEAD ** (-0.5)
    gate = jax.nn.sigmoid(gate_logit)
    query_bf = jnp.dot(tokens, w_query, preferred_element_type=jnp.float32).astype(jnp.bfloat16)
    queries = query_bf.reshape(blocks, BLK, kv_local, group, HEAD)
    keys = slot_kv[:, :, :kv_width].reshape(blocks, KP * plen, kv_local, HEAD)
    values = slot_kv[:, :, kv_width:].reshape(blocks, KP * plen, kv_local, HEAD)
    scores = (
        jnp.einsum("btkgd,bskd->bkgts", queries, keys, preferred_element_type=jnp.float32) * factor
    )
    expo = jnp.exp(scores)
    probs = expo / jnp.sum(expo, axis=-1, keepdims=True)
    probs_bf = probs.astype(jnp.bfloat16)
    attn = jnp.einsum("bkgts,bskd->btkgd", probs_bf, values, preferred_element_type=jnp.float32)
    grad_attn = out_grad.astype(jnp.float32).reshape(
        blocks, BLK, kv_local, group, HEAD
    ) * gate.reshape(kv_local, group, HEAD)
    grad_attn_bf = grad_attn.astype(jnp.bfloat16)
    grad_probs = jnp.einsum(
        "btkgd,bskd->bkgts", grad_attn_bf, values, preferred_element_type=jnp.float32
    )
    delta = jnp.moveaxis(jnp.sum(grad_attn * attn, axis=-1), 1, 3)
    grad_scores = (probs * (grad_probs - delta[..., None]) * factor).astype(jnp.bfloat16)
    grad_query = (
        jnp.einsum("bkgts,bskd->btkgd", grad_scores, keys, preferred_element_type=jnp.float32)
        .astype(jnp.bfloat16)
        .reshape(length, -1)
    )
    grad_keys = (
        jnp.einsum("bkgts,btkgd->bskd", grad_scores, queries, preferred_element_type=jnp.float32)
        .astype(jnp.bfloat16)
        .reshape(slot_count, plen, kv_width)
    )
    grad_values = (
        jnp.einsum("bkgts,btkgd->bskd", probs_bf, grad_attn_bf, preferred_element_type=jnp.float32)
        .astype(jnp.bfloat16)
        .reshape(slot_count, plen, kv_width)
    )
    slot_grad = jnp.concatenate([grad_keys, grad_values], axis=2)
    outgoing = (
        jnp.dot(placed_bf, slot_grad.reshape(slot_count, -1), preferred_element_type=jnp.float32)
        .astype(jnp.bfloat16)
        .reshape(owners, MOST, plen, 2 * kv_width)
    )
    returned = lax.all_to_all(outgoing, "st", split_axis=0, concat_axis=0, tiled=True)
    matched = (jnp.arange(pass_dev, dtype=jnp.int32)[:, None] == wanted[None, :]).astype(
        jnp.bfloat16
    )
    passage_grad = jnp.dot(
        matched, returned.reshape(cells, -1), preferred_element_type=jnp.float32
    ).reshape(pass_dev * plen, 2 * kv_width)
    key_grad = passage_grad[:, :kv_width]
    upper = key_grad.astype(jnp.bfloat16)
    lower = (key_grad - upper.astype(jnp.float32)).astype(jnp.bfloat16)
    key_term = across_rows(store_rows, upper) + across_rows(store_rows, lower)
    grad_key_weight = lax.psum(key_term, "st")
    passage_bf = passage_grad.astype(jnp.bfloat16)
    grad_store = lax.psum_scatter(
        (
            against_rows(passage_bf[:, :kv_width], w_key)
            + against_rows(passage_bf[:, kv_width:], w_value)
        ).astype(jnp.bfloat16),
        "tp",
        scatter_dimension=0,
        tiled=True,
    ).astype(jnp.float32)
    grad_store = grad_store.astype(jnp.bfloat16).reshape(-1, plen, width)
    ret_query = jnp.dot(tokens, w_ret_query, preferred_element_type=jnp.float32).astype(
        jnp.bfloat16
    )
    ret_key = jnp.dot(tokens, w_ret_key, preferred_element_type=jnp.float32).astype(jnp.bfloat16)
    ret_value = jnp.dot(tokens, w_ret_value, preferred_element_type=jnp.float32).astype(
        jnp.bfloat16
    )
    grad_rq, grad_rk, grad_rv = retention_grads(
        ret_query, ret_key, ret_value, ret_rate, ret_gain, out_grad
    )
    total = against_rows(grad_query, w_query)
    total = total + against_rows(grad_rq, w_ret_query)
    total = total + against_rows(grad_rk, w_ret_key)
    grad_tokens = lax.psum_scatter(
        (total + against_rows(grad_rv, w_ret_value)).astype(jnp.bfloat16),
        "tp",
        scatter_dimension=0,
        tiled=True,
    )
    return (grad_tokens, grad_store, grad_key_weight)


PLANE = 4
HALVES = 2
TILE = 256
BF = jnp.bfloat16
F32 = jnp.float32
MESH = pl.DeviceIdType.MESH


def nn(a, b):
    return lax.dot_general(a, b, (((1,), (0,)), ((), ())), preferred_element_type=F32)


def nt(a, b):
    return lax.dot_general(a, b, (((1,), (1,)), ((), ())), preferred_element_type=F32)


def tn(a, b):
    return lax.dot_general(a, b, (((0,), (0,)), ((), ())), preferred_element_type=F32)


def fused_kernel(
    n,
    ids_ref,
    rate_ref,
    gain_ref,
    gate_ref,
    tokens_hbm,
    store_hbm,
    wq_hbm,
    wk_hbm,
    wv_hbm,
    wrq_hbm,
    wrk_hbm,
    wrv_hbm,
    og_hbm,
    gt_hbm,
    gs_hbm,
    gkw_hbm,
    tokens,
    store,
    wq,
    wk,
    wv,
    wrq,
    wrk,
    wrv,
    og,
    q,
    rq,
    rk,
    rv,
    gq,
    grq,
    grk,
    grv,
    total,
    gt,
    gt_in,
    gs,
    gs_in,
    own_kv,
    req_out,
    req_in,
    kv_out,
    kv_in,
    stage_k,
    stage_v,
    gk_out,
    gv_out,
    gk_in,
    gv_in,
    pk,
    pv,
    slices,
    pk_in,
    p1_sum,
    p2_in,
    kg,
    owner_of,
    slot_of,
    load_sem,
    out_sem,
    tp_send,
    tp_recv,
    req_send,
    req_recv,
    kv_send,
    kv_recv,
    gk_send,
    gk_recv,
    gv_send,
    gv_recv,
    p1_send,
    p1_recv,
    pk_send,
    pk_recv,
    p2_send,
    p2_recv,
    p3_send,
    p3_recv,
    p4_send,
    p4_recv,
):
    me = lax.axis_index("st")
    tp = lax.axis_index("tp")
    length = tokens.shape[0]
    width = tokens.shape[1]
    plen = kv_in.shape[1]
    pass_dev = store.shape[0] // plen
    blocks = length // BLK
    slots = blocks * KP
    group = q.shape[1] // HEAD
    ret_heads = rate_ref.shape[0]
    depth = n // PLANE
    my_q = lax.rem(me, PLANE)
    my_z = lax.div(me, PLANE)
    half_tok = length // 2
    half_store = store.shape[0] // 2

    pairs = (
        (store_hbm, store),
        (wk_hbm, wk),
        (wv_hbm, wv),
        (tokens_hbm, tokens),
        (wrq_hbm, wrq),
        (wrk_hbm, wrk),
        (wrv_hbm, wrv),
        (og_hbm, og),
        (wq_hbm, wq),
    )
    loads = [pltpu.make_async_copy(a, b, load_sem.at[i]) for i, (a, b) in enumerate(pairs)]
    for load in loads:
        load.start()

    barrier = pltpu.get_barrier_semaphore()

    def greet(i, carry):
        pl.semaphore_signal(
            barrier, inc=1, device_id={"st": lax.rem(me + i, n)}, device_id_type=MESH
        )
        return carry

    lax.fori_loop(1, n, greet, 0)
    pl.semaphore_signal(barrier, inc=1, device_id={"tp": 1 - tp}, device_id_type=MESH)

    for s in range(slots):
        owner_of[s] = lax.div(ids_ref[s // KP, s % KP], pass_dev)

    def invert(o, carry):
        local = jnp.int32(0)
        where = jnp.int32(0)
        for s in range(slots):
            ident = ids_ref[s // KP, s % KP]
            hit = owner_of[s] == o
            local = jnp.where(hit, lax.rem(ident, pass_dev), local)
            where = jnp.where(hit, jnp.int32(s), where)
        slot_of[o] = where
        req_out[o] = jnp.full(req_out.shape[1:], local, jnp.int32)
        return carry

    lax.fori_loop(0, n, invert, 0)

    def exchange(out_ref, in_ref, send, recv, i):
        target = lax.rem(me + i, n)
        return pltpu.make_async_remote_copy(
            src_ref=out_ref.at[target],
            dst_ref=in_ref.at[me],
            send_sem=send.at[target],
            recv_sem=recv.at[me],
            device_id={"st": target},
            device_id_type=MESH,
        )

    def arrival(out_ref, in_ref, send, recv, i):
        source = lax.rem(me + i, n)
        return pltpu.make_async_remote_copy(
            src_ref=out_ref.at[source],
            dst_ref=in_ref.at[source],
            send_sem=send.at[source],
            recv_sem=recv.at[source],
            device_id={"st": source},
            device_id_type=MESH,
        )

    def start_all(*refs):
        def body(i, carry):
            exchange(*refs, i).start()
            return carry

        lax.fori_loop(1, n, body, 0)

    def wait_recv_all(*refs):
        def body(i, carry):
            arrival(*refs, i).wait_recv()
            return carry

        lax.fori_loop(1, n, body, 0)

    def wait_send_all(*refs):
        def body(i, carry):
            exchange(*refs, i).wait_send()
            return carry

        lax.fori_loop(1, n, body, 0)

    reqs = (req_out, req_in, req_send, req_recv)
    kvs = (kv_out, kv_in, kv_send, kv_recv)
    gks = (gk_out, gk_in, gk_send, gk_recv)
    gvs = (gv_out, gv_in, gv_send, gv_recv)

    pl.semaphore_wait(barrier, n)
    start_all(*reqs)
    req_in[me] = req_out[me]

    for load in loads[:3]:
        load.wait()
    own_kv[:, :HEAD] = nn(store[...], wk[...]).astype(BF)
    own_kv[:, HEAD:] = nn(store[...], wv[...]).astype(BF)
    wait_recv_all(*reqs)

    def names(r, p, lanes):
        row = jnp.where(req_in[r][0:1, :] == p, 1.0, 0.0).astype(F32)
        return jnp.concatenate([row] * (lanes // row.shape[1]), axis=1)

    def select(r, carry):
        chosen = jnp.zeros((plen, 2 * HEAD), F32)
        for p in range(pass_dev):
            chosen = chosen + names(r, p, 2 * HEAD) * own_kv[p * plen : (p + 1) * plen, :].astype(F32)
        kv_out[r] = chosen.astype(BF)
        return carry

    lax.fori_loop(0, n, select, 0)
    kv_in[me] = kv_out[me]
    start_all(*kvs)

    span = slices.shape[3]

    def columns_of(h, quarter):
        return pl.ds(pl.multiple_of((h * PLANE + quarter) * span, span), span)

    def share_rows(h, i):
        other = lax.rem(my_q + i, PLANE)
        return pltpu.make_async_remote_copy(
            src_ref=store.at[:, columns_of(h, other)],
            dst_ref=slices.at[h, i - 1],
            send_sem=p1_send.at[h, i - 1],
            recv_sem=p1_recv.at[h, i - 1],
            device_id={"st": my_z * PLANE + other},
            device_id_type=MESH,
        )

    for h in range(HALVES):
        for i in range(1, PLANE):
            share_rows(h, i).start()

    def project(w, out):
        def body(i, carry):
            cols = pl.ds(pl.multiple_of(i * TILE, TILE), TILE)
            out[:, cols] = nn(tokens[...], w[:, cols]).astype(BF)
            return carry

        lax.fori_loop(0, w.shape[1] // TILE, body, 0)

    loads[3].wait()
    for load, w, out in ((loads[4], wrq, rq), (loads[5], wrk, rk), (loads[6], wrv, rv)):
        load.wait()
        project(w, out)
    loads[7].wait()

    ret_key = rq.shape[1] // ret_heads
    ret_value = rv.shape[1] // ret_heads
    at_t = lax.broadcasted_iota(jnp.int32, (length, length), 0)
    at_s = lax.broadcasted_iota(jnp.int32, (length, length), 1)
    distance = (at_t - at_s).astype(F32)

    def retention(j, carry):
        kc = pl.ds(pl.multiple_of(j * ret_key, ret_key), ret_key)
        vc = pl.ds(pl.multiple_of(j * ret_value, ret_value), ret_value)
        damping = jnp.where(
            distance >= 0.0, jnp.exp(-rate_ref[j] * jnp.maximum(distance, 0.0)), 0.0
        ) * ret_key ** (-0.5)
        weights = (nt(rq[:, kc], rk[:, kc]) * damping).astype(BF)
        y = nn(weights, rv[:, vc])
        r = lax.rsqrt(jnp.mean(y * y, axis=1, keepdims=True) + EPSILON)
        c = og[:, vc].astype(F32) * gain_ref[:, vc]
        inner = jnp.mean(c * y, axis=1, keepdims=True)
        gy = (r * c - r * r * r * y * inner).astype(BF)
        gw = (nt(gy, rv[:, vc]) * damping).astype(BF)
        grq[:, kc] = nn(gw, rk[:, kc]).astype(BF)
        grk[:, kc] = tn(gw, rq[:, kc]).astype(BF)
        grv[:, vc] = tn(weights, gy).astype(BF)
        return carry

    lax.fori_loop(0, ret_heads, retention, 0)
    loads[8].wait()
    project(wq, q)

    def ret_total(i, carry):
        rows = pl.ds(pl.multiple_of(i * TILE, TILE), TILE)
        total[:, rows] = (
            nt(grq[...], wrq[rows, :]) + nt(grk[...], wrk[rows, :]) + nt(grv[...], wrv[rows, :])
        )
        return carry

    lax.fori_loop(0, width // TILE, ret_total, 0)

    wait_recv_all(*kvs)
    factor = HEAD ** (-0.5)

    def attend(b, carry):
        rows = pl.ds(pl.multiple_of(b * BLK, BLK), BLK)
        read = [kv_in[owner_of[b * KP + k]] for k in range(KP)]
        keys = jnp.concatenate([x[:, :HEAD] for x in read], axis=0)
        values = jnp.concatenate([x[:, HEAD:] for x in read], axis=0)
        cols = [slice(g * HEAD, (g + 1) * HEAD) for g in range(group)]
        queries = jnp.concatenate([q[rows, c] for c in cols], axis=0)
        expo = jnp.exp(nt(queries, keys) * factor)
        probs = expo / jnp.sum(expo, axis=1, keepdims=True)
        probs_bf = probs.astype(BF)
        attn = nn(probs_bf, values)
        grad_attn = jnp.concatenate(
            [
                og[rows, c].astype(F32) * (1.0 / (1.0 + jnp.exp(-gate_ref[:, c])))
                for c in cols
            ],
            axis=0,
        )
        grad_attn_bf = grad_attn.astype(BF)
        grad_probs = nt(grad_attn_bf, values)
        delta = jnp.sum(grad_attn * attn, axis=1, keepdims=True)
        scores = (probs * (grad_probs - delta) * factor).astype(BF)
        grad_query = nn(scores, keys).astype(BF)
        for g, c in enumerate(cols):
            gq[rows, c] = grad_query[g * BLK : (g + 1) * BLK, :]
        dk = tn(scores, queries).astype(BF)
        dv = tn(probs_bf, grad_attn_bf).astype(BF)
        for k in range(KP):
            stage_k[b * KP + k] = dk[k * plen : (k + 1) * plen, :]
            stage_v[b * KP + k] = dv[k * plen : (k + 1) * plen, :]
        return carry

    lax.fori_loop(0, blocks, attend, 0)

    def place(stage, out):
        def body(o, carry):
            out[o] = stage[slot_of[o]]
            return carry

        lax.fori_loop(0, n, body, 0)

    place(stage_k, gk_out)
    place(stage_v, gv_out)
    gk_in[me] = gk_out[me]
    gv_in[me] = gv_out[me]
    start_all(*gks)
    start_all(*gvs)

    def finish_total(i, carry):
        rows = pl.ds(pl.multiple_of(i * TILE, TILE), TILE)
        gt[:, rows] = (total[:, rows] + nt(gq[...], wq[rows, :])).astype(BF)
        return carry

    lax.fori_loop(0, width // TILE, finish_total, 0)

    def to_partner(out_ref, in_ref, half, at):
        return pltpu.make_async_remote_copy(
            src_ref=out_ref.at[pl.ds(pl.multiple_of((1 - tp) * half, half), half)],
            dst_ref=in_ref,
            send_sem=tp_send.at[at],
            recv_sem=tp_recv.at[at],
            device_id={"tp": 1 - tp},
            device_id_type=MESH,
        )

    def add_own(out_ref, in_ref, half):
        own = out_ref[pl.ds(pl.multiple_of(tp * half, half), half), :]
        in_ref[...] = (own.astype(F32) + in_ref[...].astype(F32)).astype(BF)

    token_swap = to_partner(gt, gt_in, half_tok, 0)
    token_swap.start()

    def gather_sum(in_ref, out_ref):
        for p in range(pass_dev):

            def body(r, acc):
                return acc + names(r, p, HEAD) * in_ref[r].astype(F32)

            acc = lax.fori_loop(0, n, body, jnp.zeros((plen, HEAD), F32))
            out_ref[p * plen : (p + 1) * plen, :] = acc.astype(BF)

    wait_recv_all(*gks)
    gather_sum(gk_in, pk)
    def chunk(h, quarter):
        return pl.ds((h * PLANE + quarter) * depth, depth)

    def share_key(i):
        return pltpu.make_async_remote_copy(
            src_ref=pk,
            dst_ref=pk_in.at[i - 1],
            send_sem=pk_send.at[i - 1],
            recv_sem=pk_recv.at[i - 1],
            device_id={"st": my_z * PLANE + lax.rem(my_q + i, PLANE)},
            device_id_type=MESH,
        )

    def column_reduce(h, i):
        other = lax.rem(my_z + i, depth)
        return pltpu.make_async_remote_copy(
            src_ref=p1_sum.at[h, other],
            dst_ref=p2_in.at[h, i - 1],
            send_sem=p2_send.at[h, i - 1],
            recv_sem=p2_recv.at[h, i - 1],
            device_id={"st": other * PLANE + my_q},
            device_id_type=MESH,
        )

    def column_gather(h, i, source):
        at = kg.at[(h * PLANE + my_q) * depth + source]
        return pltpu.make_async_remote_copy(
            src_ref=at,
            dst_ref=at,
            send_sem=p3_send.at[h, i - 1],
            recv_sem=p3_recv.at[h, i - 1],
            device_id={"st": lax.rem(my_z + i, depth) * PLANE + my_q},
            device_id_type=MESH,
        )

    def plane_gather(h, i, source):
        at = kg.at[chunk(h, source)]
        return pltpu.make_async_remote_copy(
            src_ref=at,
            dst_ref=at,
            send_sem=p4_send.at[h, i - 1],
            recv_sem=p4_recv.at[h, i - 1],
            device_id={"st": my_z * PLANE + lax.rem(my_q + i, PLANE)},
            device_id_type=MESH,
        )

    for i in range(1, PLANE):
        share_key(i).start()
    own_terms = [tn(store[:, columns_of(h, my_q)], pk[...]) for h in range(HALVES)]

    token_swap.wait_recv()
    add_own(gt, gt_in, half_tok)
    token_out = pltpu.make_async_copy(gt_in, gt_hbm, out_sem.at[0])
    token_out.start()

    for i in range(1, PLANE):
        share_key(i).wait_recv()
        for h in range(HALVES):
            share_rows(h, i).wait_recv()
    for h in range(HALVES):
        acc = own_terms[h]
        for i in range(1, PLANE):
            acc = acc + tn(slices[h, i - 1], pk_in[i - 1])
        acc = acc.reshape(p1_sum.shape[1:])
        p1_sum[h] = acc.astype(BF)
        for i in range(1, depth):
            column_reduce(h, i).start()

    wait_recv_all(*gvs)
    gather_sum(gv_in, pv)

    def store_grad(i, carry):
        rows = pl.ds(pl.multiple_of(i * TILE, TILE), TILE)
        gs[:, rows] = (nt(pk[...], wk[rows, :]) + nt(pv[...], wv[rows, :])).astype(BF)
        return carry

    lax.fori_loop(0, width // TILE, store_grad, 0)
    store_swap = to_partner(gs, gs_in, half_store, 1)
    store_swap.start()

    for h in range(HALVES):
        for i in range(1, depth):
            column_reduce(h, i).wait_recv()
        acc = p1_sum[h, my_z].astype(F32)
        for i in range(1, depth):
            acc = acc + p2_in[h, i - 1].astype(F32)
        kg[(h * PLANE + my_q) * depth + my_z] = acc.astype(BF)
        for i in range(1, depth):
            column_gather(h, i, my_z).start()

    store_swap.wait_recv()
    add_own(gs, gs_in, half_store)
    store_out = pltpu.make_async_copy(gs_in, gs_hbm, out_sem.at[1])
    store_out.start()

    for h in range(HALVES):
        for i in range(1, depth):
            column_gather(h, i, lax.rem(my_z + depth - i, depth)).wait_recv()
        for i in range(1, PLANE):
            plane_gather(h, i, my_q).start()
    for h in range(HALVES):
        for i in range(1, PLANE):
            plane_gather(h, i, lax.rem(my_q + PLANE - i, PLANE)).wait_recv()
    weight_out = pltpu.make_async_copy(kg, gkw_hbm, out_sem.at[2])
    weight_out.start()

    wait_send_all(*reqs)
    wait_send_all(*kvs)
    wait_send_all(*gks)
    wait_send_all(*gvs)
    token_swap.wait_send()
    store_swap.wait_send()
    for h in range(HALVES):
        for i in range(1, PLANE):
            share_rows(h, i).wait_send()
            plane_gather(h, i, my_q).wait_send()
        for i in range(1, depth):
            column_reduce(h, i).wait_send()
            column_gather(h, i, my_z).wait_send()
    for i in range(1, PLANE):
        share_key(i).wait_send()
    token_out.wait()
    store_out.wait()
    weight_out.wait()


def per_device(sizes, *args):
    (tokens, store, ids, wq, wk, wv, wrq, wrk, wrv, rate, gain, gate, og) = args
    n = sizes["st"]
    pass_dev, plen, width = store.shape
    length = tokens.shape[0]
    rows = pass_dev * plen
    weight_cols = sum(w.shape[1] for w in (wq, wk, wv, wrq, wrk, wrv))
    fits = (
        sizes["tp"] == 2
        and wk.shape[1] == HEAD
        and ids.size == n
        and n % PLANE == 0
        and width % (HALVES * n) == 0
        and width % (HALVES * PLANE * 128) == 0
        and width // (HALVES * n) % 16 == 0
        and width * weight_cols + n * plen * HEAD * 12 + length * width * 12 < 24 * 2**20
    )
    if not fits:
        return per_device_plain(*args)
    depth = n // PLANE
    piece = width // (HALVES * n)

    def vm(*shape, dtype=BF):
        return pltpu.VMEM(shape, dtype)

    any_spec = pl.BlockSpec(memory_space=pl.ANY)
    smem = pl.BlockSpec(memory_space=pltpu.SMEM)
    vmem = pl.BlockSpec(memory_space=pltpu.VMEM)
    dma = pltpu.SemaphoreType.DMA
    like = [vm(*x.shape) for x in (tokens,)] + [vm(rows, width)]
    like += [vm(*x.shape) for x in (wq, wk, wv, wrq, wrk, wrv, og)]
    qs = [vm(length, w.shape[1]) for w in (wq, wrq, wrk, wrv)]
    scratch = (
        like
        + qs
        + qs
        + [
            vm(length, width, dtype=F32),
            vm(length, width),
            vm(length // 2, width),
            vm(rows, width),
            vm(rows // 2, width),
            vm(rows, 2 * HEAD),
            vm(n, 8, 128, dtype=jnp.int32),
            vm(n, 8, 128, dtype=jnp.int32),
            vm(n, plen, 2 * HEAD),
            vm(n, plen, 2 * HEAD),
        ]
        + [vm(n, plen, HEAD)] * 6
        + [
            vm(rows, HEAD),
            vm(rows, HEAD),
            vm(HALVES, PLANE - 1, rows, width // (HALVES * PLANE)),
            vm(PLANE - 1, rows, HEAD),
            vm(HALVES, depth, piece, HEAD),
            vm(HALVES, depth - 1, piece, HEAD),
            vm(HALVES * n, piece, HEAD),
            pltpu.SMEM((n,), jnp.int32),
            pltpu.SMEM((n,), jnp.int32),
            dma((9,)),
            dma((3,)),
            dma((2,)),
            dma((2,)),
        ]
        + [dma((n,))] * 8
        + [dma((HALVES, PLANE - 1))] * 2
        + [dma((PLANE - 1,))] * 2
        + [dma((HALVES, depth - 1))] * 4
        + [dma((HALVES, PLANE - 1))] * 2
    )
    grad_tokens, grad_store, grad_key = pl.pallas_call(
        functools.partial(fused_kernel, n),
        out_shape=(
            jax.ShapeDtypeStruct((length // 2, width), BF),
            jax.ShapeDtypeStruct((rows // 2, width), BF),
            jax.ShapeDtypeStruct((HALVES * n, piece, HEAD), BF),
        ),
        in_specs=[smem, smem, vmem, vmem] + [any_spec] * 9,
        out_specs=(any_spec, any_spec, any_spec),
        scratch_shapes=scratch,
        compiler_params=pltpu.CompilerParams(
            collective_id=0, has_side_effects=True, vmem_limit_bytes=60 * 2**20
        ),
    )(
        ids,
        rate,
        gain.reshape(1, -1),
        gate.reshape(1, -1),
        tokens,
        store.reshape(rows, width),
        wq,
        wk,
        wv,
        wrq,
        wrk,
        wrv,
        og,
    )
    return (
        grad_tokens,
        grad_store.reshape(pass_dev // 2, plen, width),
        grad_key.reshape(width, HEAD).astype(F32),
    )


def solution(mesh):
    return jax.shard_map(
        functools.partial(per_device, dict(mesh.shape)),
        mesh=mesh,
        in_specs=(
            P("st", None),
            P("st", None, None),
            P("st", None),
            P(None, "tp"),
            P(None, "tp"),
            P(None, "tp"),
            P(None, "tp"),
            P(None, "tp"),
            P(None, "tp"),
            P("tp"),
            P("tp"),
            P("tp"),
            P("st", "tp"),
        ),
        out_specs=(P(("st", "tp"), None), P(("st", "tp"), None, None), P(None, "tp")),
        check_vma=False,
    )
```
